512 devices in a mesh: sp: 32 (over z, x), tp: 16 (over y, core).
Axes of the slice: x: 4, y: 8, z: 8, core: 2. Of those that a mesh axis runs over, the one named last changes fastest.
Arguments:
- ffn_input: bfloat16 [4096, 2048], P('sp', 'tp'), may hold values from -6 to 6
- out_grad: bfloat16 [4096, 2048], P('sp', 'tp'), may hold values from -6 to 6
- routes: int32 [4096, 2], P('sp'), may hold values from 0 to 31, all different within a row; in each aligned block of 128 rows (0 to 127, 128 to 255, ...) at most 10 rows name the same one
- route_weight: float32 [4096, 2], P('sp'), may hold values from 0.05 to 1
- gate_w: bfloat16 [32, 2048, 2048], P('sp', None, 'tp'), may hold values from -0.125 to 0.125
- up_w: bfloat16 [32, 2048, 2048], P('sp', None, 'tp'), may hold values from -0.125 to 0.125
- down_w: bfloat16 [32, 2048, 2048], P('sp', 'tp'), may hold values from -0.125 to 0.125
- out_proj: bfloat16 [2048, 2048], P('tp'), may hold values from -0.125 to 0.125
- rec_value: bfloat16 [4096, 2048], P('sp', 'tp'), may hold values from -6 to 6
- rate_pre: bfloat16 [4096, 2048], P('sp', 'tp'), may hold values from -6 to 6
- input_pre: bfloat16 [4096, 2048], P('sp', 'tp'), may hold values from -4 to 4
- prev_state: bfloat16 [4096, 2048], P('sp', 'tp'), may hold values from -6 to 6
- decay_param: float32 [2048], P('tp'), may hold values from 4 to 12
Outputs:
- gate_w_grad: bfloat16 [32, 2048, 2048], P('sp', None, 'tp')
- up_w_grad: bfloat16 [32, 2048, 2048], P('sp', None, 'tp')
- down_w_grad: bfloat16 [32, 2048, 2048], P('sp', 'tp')
- out_proj_grad: float32 [2048, 2048], P('sp', 'tp')
- rec_value_grad: bfloat16 [4096, 2048], P('sp', 'tp')
- rate_pre_grad: bfloat16 [4096, 2048], P('sp', 'tp')
- input_pre_grad: bfloat16 [4096, 2048], P('sp', 'tp')
The draws below stay inside these ranges and needn't reach their ends.
Inputs may be any that keep to these rules, and one draw needn't show every extreme that they name: `routes`: each token names 2 different experts. Within each aligned block of 128 tokens no expert is named more than 10 times, a bound that some block reaches.
All inputs are finite; a program needn't handle non-finite values.
Results may differ from the reference program's by a relative error of at most 0.02.
Values may be sent and summed in bfloat16 or wider, within the bound.
A program may use at most 64 MiB of HBM per device.

```python
import math
import jax
import jax.numpy as jnp
import numpy as np
from jax import lax

D = 2048
DR = 2048
FF_E = 2048
TOP = 2
TOK_DEV = 128
EXPERTS = 32
TOKENS = 4096
CAP = 10
N_SP = 32
N_TP = 16


def draw_rate_pre(key, part):
    noise_key = jax.random.fold_in(key, 11)
    block_key = jax.random.fold_in(key, 12)
    blocks = (TOKENS + 127) // 128
    offsets = jax.random.uniform(block_key, (blocks, 1), jnp.float32, -2.0, 2.0)
    position_block = jnp.arange(TOKENS) // 128
    base_noise = jax.random.normal(noise_key, (TOKENS, DR), jnp.float32)
    return jnp.clip(base_noise + offsets[position_block], -6.0, 6.0).astype(jnp.bfloat16)


def draw_decay_param(key, part):
    pick_key = jax.random.fold_in(key, 21)
    fast_key = jax.random.fold_in(key, 22)
    slow_key = jax.random.fold_in(key, 23)
    fast_share = 0.5
    is_fast = jax.random.bernoulli(pick_key, fast_share, (DR,))
    fast_rate = jnp.exp(jax.random.uniform(fast_key, (DR,), jnp.float32, jnp.log(0.004), jnp.log(0.012)))
    slow_rate = jnp.exp(jax.random.uniform(slow_key, (DR,), jnp.float32, jnp.log(0.1 / TOKENS), jnp.log(0.4 / TOKENS)))
    speed_value = jnp.where(is_fast, fast_rate, slow_rate)
    return (-jnp.log(jnp.expm1(speed_value))).astype(jnp.float32)


def with_spikes(drawn, rng, source, target, parts, factor):
    def block_of(dim):
        return (jnp.arange(drawn.shape[dim]) // (drawn.shape[dim] // parts)).reshape((-1,) + (1,) * (drawn.ndim - 1 - dim))

    one_side = jax.random.permutation(rng, parts)[block_of(target)]
    far = (block_of(target) + parts // 2) % parts
    return jnp.where((block_of(source) == one_side) | (block_of(source) == far), factor * drawn, drawn)


def levels(stream_key, shape, cuts, low, high):
    def one(dim, shards_of):
        steps = jax.random.uniform(jax.random.fold_in(jax.random.fold_in(stream_key, 6), dim), (shards_of,), jnp.float32, low / len(cuts), high / len(cuts))
        return jnp.repeat(jnp.exp(steps), shape[dim] // shards_of).reshape((-1,) + (1,) * (len(shape) - dim - 1))

    level = one(*cuts[0])
    for cut in cuts[1:]:
        level = level * one(*cut)
    return level


def deal_out(stream_key, own, number, rows, number_of, top, bound, skew):
    order = jax.random.permutation(stream_key, number_of)
    heavy_load, common = portions_of(number_of, rows * top, bound, skew, True), portions_of(number_of, rows * top, bound, skew, False)
    places = jnp.arange(number_of)

    def named(sizes, offset_by):
        used = int((sizes > 0).sum())
        fixed = max(1, used // 4)
        shifted = fixed + (places - fixed + offset_by * (used - fixed)) % max(1, number_of - fixed)
        return jnp.zeros((number_of,), jnp.int32).at[order[jnp.where(places < fixed, places, shifted)]].set(jnp.asarray(sizes, jnp.int32))

    sizes = jnp.where(number % 4 == 0, named(heavy_load, number // 4), named(common, number - number // 4 - 1))
    mixed = jax.random.permutation(jax.random.fold_in(own, 3), number_of)
    source_of, receiver = mixed[0:number_of // 2 * 2:2], mixed[1:number_of // 2 * 2:2]
    slack = jnp.minimum(sizes[source_of] - 1, bound - sizes[receiver]) // 2
    slack = jnp.where((source_of == order[0]) | (receiver == order[0]) | (sizes[receiver] == 0), 0, jnp.maximum(slack, 0))
    shifted = jax.random.randint(jax.random.fold_in(own, 4), (number_of // 2,), 0, 1 << 20) % (slack + 1)
    sizes = sizes.at[source_of].add(-shifted).at[receiver].add(shifted)
    labels = jnp.searchsorted(jnp.cumsum(sizes), jnp.arange(rows * top), side="right").astype(jnp.int32)
    table = labels.reshape(top, rows).T
    table = table[jax.random.permutation(jax.random.fold_in(own, 1), rows)]
    offset_by = jax.random.randint(jax.random.fold_in(own, 2), (rows, 1), 0, top)
    return jnp.take_along_axis(table, (jnp.arange(top)[None, :] + offset_by) % top, axis=1)


def portions_of(number_of, total, bound, skew, full):
    portions = [(1 << 20) // math.isqrt(standing ** skew) + 1 for standing in range(1, number_of + 1)]
    largest = bound if full else min(bound, max(-(-total // number_of), total * portions[0] // sum(portions)))
    least = 1 if total - largest >= number_of - 1 else 0
    counts, surplus = [largest] + [least] * (number_of - 1), total - largest - least * (number_of - 1)
    while surplus > 0:
        candidates = [i for i in range(1, number_of) if counts[i] < largest] or [i for i in range(1, number_of) if counts[i] < bound]
        mass, remaining = sum([portions[i] for i in candidates]), surplus
        for i in candidates:
            more = min(bound - counts[i], max(1, remaining * portions[i] // mass), surplus)
            counts[i] = counts[i] + more
            surplus = surplus - more
    return np.array(counts)


def normal_values(key, extent, width, limit, split=(), held_as=jnp.bfloat16):
    array = jax.random.normal(key, extent, jnp.float32) * width
    if len(split) > 0:
        array = levels(key, extent, split, -0.22, 0.18) * array
    return jnp.clip(array, min=-limit, max=limit).astype(held_as)


def heavy_noise(rng, dims, scale, limit, pieces, heavy, kind=jnp.bfloat16):
    values = scale * jax.random.normal(rng, dims, jnp.float32)
    if pieces:
        values = values * levels(rng, dims, pieces, -0.22, 0.18)
    return jnp.clip(with_spikes(values, jax.random.fold_in(rng, 3), *heavy), -limit, limit).astype(kind)


def setup_inputs(seed: int = 0) -> dict:
    key_of = jax.random.split(jax.random.key(seed), 14)
    ffn_input = normal_values(key_of[0], (TOKENS, D), 1.0, 6.0, ((0, 32), (1, 16)))
    out_grad = heavy_noise(key_of[1], (TOKENS, D), 1.0, 6.0, ((0, 32), (1, 16)), (0, 1, 32, 2.75))
    routes_keys = jax.random.split(jax.random.fold_in(key_of[2], 1), TOKENS // TOK_DEV)
    routes_turns = jax.random.permutation(jax.random.fold_in(key_of[2], 3), TOKENS // TOK_DEV)
    routes = jax.vmap(lambda own, number: deal_out(jax.random.fold_in(key_of[2], 2), own, number, TOK_DEV, EXPERTS, TOP, CAP, 1))(routes_keys, routes_turns).reshape((TOKENS, TOP))
    route_weight = jnp.clip(0.05 + 0.95 * jax.random.uniform(key_of[3], (TOKENS, TOP), jnp.float32) ** levels(key_of[3], (TOKENS, TOP), ((0, 32),), -0.2, 0.2), 0.05, 1.0)
    gate_w = normal_values(key_of[4], (EXPERTS, D, FF_E), D ** -0.5, 0.125, ((0, 32), (2, 16)))
    up_w = normal_values(key_of[5], (EXPERTS, D, FF_E), D ** -0.5, 0.125, ((0, 32), (2, 16)))
    down_w = normal_values(key_of[6], (EXPERTS, FF_E, D), FF_E ** -0.5, 0.125, ((0, 32), (1, 16)))
    out_proj = normal_values(key_of[7], (DR, D), DR ** -0.5, 0.125, ((0, 16),))
    rec_value = normal_values(key_of[8], (TOKENS, DR), 1.0, 6.0, ((0, 32), (1, 16)))
    rate_pre = draw_rate_pre(jax.random.fold_in(key_of[13], 71), 0)
    input_pre = normal_values(key_of[10], (TOKENS, DR), 1.0, 4.0, ((0, 32), (1, 16)))
    prev_state = normal_values(key_of[11], (TOKENS, DR), 1.0, 6.0, ((0, 32), (1, 16)))
    decay_param = draw_decay_param(jax.random.fold_in(key_of[13], 71), 0)
    return {"ffn_input": ffn_input, "out_grad": out_grad, "routes": routes, "route_weight": route_weight, "gate_w": gate_w, "up_w": up_w, "down_w": down_w, "out_proj": out_proj, "rec_value": rec_value, "rate_pre": rate_pre, "input_pre": input_pre, "prev_state": prev_state, "decay_param": decay_param}


decay_scale = 8.0

def chain_link(left_pair, right_pair):
    return (left_pair[0] * right_pair[0], right_pair[0] * left_pair[1] + right_pair[1])

def expert_pass(rows_in, rows_cot, w_gate, w_up, w_down):
    gate_act = jnp.dot(rows_in, w_gate, preferred_element_type=jnp.float32)
    up_act = jnp.dot(rows_in, w_up, preferred_element_type=jnp.float32)
    squash = jax.nn.sigmoid(gate_act)
    silu_gate = gate_act * squash
    hidden = (silu_gate * up_act).astype(jnp.bfloat16)
    down_grad = jnp.dot(hidden.T, rows_cot, preferred_element_type=jnp.float32).astype(jnp.bfloat16)
    hidden_grad = jnp.dot(rows_cot, w_down.T, preferred_element_type=jnp.float32)
    gate_grad = (hidden_grad * up_act * squash * (1.0 + gate_act * (1.0 - squash))).astype(jnp.bfloat16)
    up_grad = (hidden_grad * silu_gate).astype(jnp.bfloat16)
    gate_w_grad = jnp.dot(rows_in.T, gate_grad, preferred_element_type=jnp.float32).astype(jnp.bfloat16)
    up_w_grad = jnp.dot(rows_in.T, up_grad, preferred_element_type=jnp.float32).astype(jnp.bfloat16)
    group_width = gate_grad.shape[1] // N_TP
    model_width = w_gate.shape[0]
    gate_parts = jnp.einsum('rjf,djf->jrd', gate_grad.reshape(-1, N_TP, group_width).astype(jnp.float32), w_gate.reshape(model_width, N_TP, group_width).astype(jnp.float32))
    up_parts = jnp.einsum('rjf,djf->jrd', up_grad.reshape(-1, N_TP, group_width).astype(jnp.float32), w_up.reshape(model_width, N_TP, group_width).astype(jnp.float32))
    group_parts = lax.optimization_barrier((gate_parts + up_parts).astype(jnp.bfloat16))
    row_grad = lax.optimization_barrier(jnp.sum(group_parts.astype(jnp.float32), axis=0)).astype(jnp.bfloat16)
    return (gate_w_grad, up_w_grad, down_grad, row_grad)

def reference(ffn_input, out_grad, routes, route_weight, gate_w, up_w, down_w, out_proj, rec_value, rate_pre, input_pre, prev_state, decay_param):
    slot_total = EXPERTS * N_SP * CAP
    flat_routes = routes.reshape(N_SP, TOK_DEV * TOP)
    route_marks = (flat_routes[:, :, None] == jnp.arange(EXPERTS, dtype=jnp.int32)[None, None, :]).astype(jnp.int32)
    before = lax.optimization_barrier(jnp.sum((jnp.cumsum(route_marks, axis=1) - route_marks) * route_marks, axis=2))
    source = jnp.arange(N_SP, dtype=jnp.int32)[:, None]
    slot_index = (flat_routes * (N_SP * CAP) + source * CAP + before).reshape(-1).astype(jnp.int32)
    route_ids = jnp.arange(TOKENS * TOP, dtype=jnp.int32)
    slot_owner = jnp.zeros((slot_total,), jnp.int32).at[slot_index].set(route_ids)
    filled = jnp.zeros((slot_total,), jnp.int32).at[slot_index].set(1)
    flat_weight = route_weight.reshape(-1)

    def one_expert(expert_items):
        w_gate, w_up, w_down, owned_route, filled_row = expert_items
        token_index = owned_route // TOP
        kept_mask = filled_row[:, None] > 0
        rows_in = jnp.where(kept_mask, ffn_input[token_index], jnp.zeros((), jnp.bfloat16))
        scaled = (flat_weight[owned_route][:, None] * out_grad[token_index].astype(jnp.float32)).astype(jnp.bfloat16)
        rows_cot = jnp.where(kept_mask, scaled, jnp.zeros((), jnp.bfloat16))
        return expert_pass(rows_in, rows_cot, w_gate, w_up, w_down)
    gate_w_grad, up_w_grad, down_w_grad, row_grad = lax.map(one_expert, (gate_w, up_w, down_w, slot_owner.reshape(EXPERTS, N_SP * CAP), filled.reshape(EXPERTS, N_SP * CAP)))
    picked = row_grad.reshape(slot_total, D)[slot_index].astype(jnp.float32).reshape(TOKENS, TOP, D)
    mix_grad = (lax.optimization_barrier(jnp.sum(picked, axis=1)) + out_grad.astype(jnp.float32)).astype(jnp.bfloat16)
    state_grad = jnp.dot(mix_grad, out_proj.T, preferred_element_type=jnp.float32)
    rate_gate = jax.nn.sigmoid(rate_pre.astype(jnp.float32))
    input_gate = jax.nn.sigmoid(input_pre.astype(jnp.float32))
    decay_speed = jax.nn.softplus(-decay_param.astype(jnp.float32))[None, :]
    log_decay = -decay_scale * rate_gate * decay_speed
    decay = jnp.exp(log_decay)
    scale_in = jnp.sqrt(-jnp.expm1(2.0 * log_decay))
    signal = rec_value.astype(jnp.float32)
    before_state = prev_state.astype(jnp.float32)
    rec_state = (decay * before_state + scale_in * input_gate * signal).astype(jnp.bfloat16)
    out_proj_grad = jnp.dot(mix_grad.T, rec_state, preferred_element_type=jnp.float32)
    following = jnp.concatenate([decay[1:], jnp.ones((1, DR), jnp.float32)], axis=0)
    _, carried = lax.associative_scan(chain_link, (following[::-1], state_grad[::-1]), axis=0)
    carried = carried[::-1]
    rec_value_grad = (carried * scale_in * input_gate).astype(jnp.bfloat16)
    input_pre_grad = (carried * scale_in * signal * input_gate * (1.0 - input_gate)).astype(jnp.bfloat16)
    decay_part = decay * before_state - input_gate * signal * decay * decay / scale_in
    rate_pre_grad = (carried * decay_part * (-decay_scale * decay_speed) * rate_gate * (1.0 - rate_gate)).astype(jnp.bfloat16)
    return (gate_w_grad, up_w_grad, down_w_grad, out_proj_grad, rec_value_grad, rate_pre_grad, input_pre_grad)
```

```python
import functools

import jax
import jax.numpy as jnp
from jax import lax
from jax.experimental import pallas as pl
from jax.experimental.pallas import tpu as pltpu
from jax.sharding import PartitionSpec as P

MESH = pl.DeviceIdType.MESH
F32 = jnp.float32
BF = jnp.bfloat16
decay_scale = 8.0
SLOT_PAD = 16
LANES = 128


def dot(a, b, ca, cb):
    return lax.dot_general(a, b, (((ca,), (cb,)), ((), ())), preferred_element_type=F32)


def expm1_neg(v):
    near = jnp.ones_like(v)
    for n in range(9, 1, -1):
        near = 1.0 + v * near * (1.0 / n)
    return jnp.where(v > -0.5, v * near, jnp.exp(v) - 1.0)


def step_kernel(
    dims,
    x_ref,
    cot_ref,
    rt_ref,
    rw_ref,
    gw_hbm,
    uw_hbm,
    dw_hbm,
    op_hbm,
    rv_ref,
    rp_ref,
    ip_ref,
    ps_ref,
    dp_ref,
    gwg_hbm,
    uwg_hbm,
    dwg_hbm,
    opg_ref,
    rvg_ref,
    rpg_ref,
    ipg_ref,
    wgu,
    wpart,
    dw,
    op,
    onehot,
    send1,
    recv1,
    inf,
    cotf,
    acc,
    hacc,
    grads,
    grads_p,
    hid,
    part,
    rss,
    rsr,
    send5,
    recv5,
    mixf,
    sg,
    levels,
    through,
    coef,
    rec,
    xsend,
    xrecv,
    zsend,
    zrecv,
    chs,
    chr_,
    ogu,
    odw,
    w_sem,
    o_sem,
    wp_s,
    wp_r,
    p1_s,
    p1_r,
    y_s,
    y_r,
    d_s,
    d_r,
    g_s,
    g_r,
    q_s,
    q_r,
    p5_s,
    p5_r,
    m_s,
    m_r,
    md_s,
    md_r,
    x_s,
    x_r,
    z_s,
    z_r,
    c_s,
    c_r,
):
    SPN, NX, NY, E, CAP, TD, R = dims
    NZ = SPN // NX
    RH = R // 2
    EH = E // 2
    CP = SLOT_PAD
    H = NY // 2
    s = lax.axis_index("sp")
    t = lax.axis_index("tp")
    y = t // 2
    c = t % 2
    z = s // NX
    x = s % NX

    def remote(src, dst, ss, rs, dev):
        return pltpu.make_async_remote_copy(
            src_ref=src, dst_ref=dst, send_sem=ss, recv_sem=rs, device_id=dev, device_id_type=MESH
        )

    def at_y(j):
        return (s, lax.rem(y + j + NY, NY) * 2 + c)

    partner = (s, y * 2 + 1 - c)

    def at_sp(j):
        return (lax.rem(s + j + SPN, SPN), t)

    def took(ref, sem):
        pltpu.make_async_copy(ref, ref, sem).wait()

    barrier = pltpu.get_barrier_semaphore()

    def greet(k, carry):
        pl.semaphore_signal(barrier, inc=1, device_id=at_sp(k), device_id_type=MESH)
        return carry

    lax.fori_loop(1, SPN, greet, 0)
    for j in range(1, NY):
        pl.semaphore_signal(barrier, inc=1, device_id=at_y(j), device_id_type=MESH)
    pl.semaphore_signal(barrier, inc=1, device_id=partner, device_id_type=MESH)

    loads = [
        pltpu.make_async_copy(gw_hbm, wgu.at[:, pl.ds(0, LANES)], w_sem.at[0]),
        pltpu.make_async_copy(uw_hbm, wgu.at[:, pl.ds(LANES, LANES)], w_sem.at[1]),
        pltpu.make_async_copy(dw_hbm, dw, w_sem.at[2]),
        pltpu.make_async_copy(op_hbm, op, w_sem.at[3]),
    ]
    for load in loads:
        load.start()

    rows = lax.broadcasted_iota(jnp.int32, (TD, TD), 0)
    cols = lax.broadcasted_iota(jnp.int32, (TD, TD), 1)
    earlier = (rows > cols).astype(BF)
    lane = lax.broadcasted_iota(jnp.int32, (TD, LANES), 1)
    r0, r1 = rt_ref[:, 0:1], rt_ref[:, 1:2]
    marks0 = (lane == r0).astype(F32)
    marks1 = (lane == r1).astype(F32)
    before = dot(earlier, (marks0 + marks1).astype(BF), 1, 0)
    slots = lax.broadcasted_iota(jnp.int32, (TD, E * CP), 1)

    def picks(r, marks):
        rank = jnp.sum(before * marks, axis=1, keepdims=True).astype(jnp.int32)
        away = jnp.where(r <= s, s - r, s - r + SPN)
        return (slots == away * CP + rank).astype(F32)

    pick0 = picks(r0, marks0)
    pick1 = picks(r1, marks1)
    both = (pick0 + pick1).astype(BF)
    onehot[...] = both
    cot = cot_ref[...].astype(F32)
    sc0 = (rw_ref[:, 0:1] * cot).astype(BF)
    sc1 = (rw_ref[:, 1:2] * cot).astype(BF)
    row_in = dot(both, x_ref[...], 0, 0).astype(BF)
    row_cot = (dot(pick0.astype(BF), sc0, 0, 0) + dot(pick1.astype(BF), sc1, 0, 0)).astype(BF)
    send1[:, :, 0:LANES] = row_in.reshape(E, CP, LANES)
    send1[:, :, LANES:] = row_cot.reshape(E, CP, LANES)
    recv1[0] = send1[0]

    pl.semaphore_wait(barrier, SPN - 1 + NY - 1 + 1)

    def all_sent(src_of, dst_of, ss, rs, sign):
        def go(k):
            remote(src_of(k), dst_of(k), ss, rs, at_sp(sign * k)).start()

        def pair(k, carry):
            go(k)
            go(SPN - k)
            return carry

        lax.fori_loop(1, SPN // 2, pair, 0)
        go(SPN // 2)

    all_sent(lambda k: send1.at[k], lambda k: recv1.at[k], p1_s, p1_r, -1)

    loads[0].wait()
    loads[1].wait()
    for j in range(NY):
        remote(
            wgu.at[pl.ds(pl.multiple_of(j * 256 + (1 - c) * LANES, LANES), LANES), :],
            wpart.at[j],
            wp_s,
            wp_r,
            partner,
        ).start()
    loads[2].wait()
    loads[3].wait()

    decay_speed = jnp.log1p(jnp.exp(-dp_ref[...]))
    rate = jax.nn.sigmoid(rp_ref[...].astype(F32))
    inlet = jax.nn.sigmoid(ip_ref[...].astype(F32))
    signal = rv_ref[...].astype(F32)
    prev = ps_ref[...].astype(F32)
    log_decay = -decay_scale * rate * decay_speed
    decay = jnp.exp(log_decay)
    scale_in = jnp.sqrt(-expm1_neg(2.0 * log_decay))
    rec[...] = (decay * prev + scale_in * inlet * signal).astype(BF)
    gain = scale_in * inlet
    coef[0] = gain
    coef[1] = gain * signal * (1.0 - inlet)
    slope = decay * prev - inlet * signal * decay * decay / scale_in
    coef[2] = slope * (-decay_scale * decay_speed) * rate * (1.0 - rate)
    tok = lax.broadcasted_iota(jnp.int32, (TD, LANES), 0)
    span = jnp.where(tok < TD - 1, pltpu.roll(decay, TD - 1, 0), 1.0)
    n_levels = TD.bit_length() - 1
    for k in range(n_levels):
        inside = tok < TD - (1 << k)
        levels[k] = jnp.where(inside, span, 0.0)
        span = span * jnp.where(inside, pltpu.roll(span, TD - (1 << k), 0), 1.0)
    through[...] = span
    first_decay = decay[0:1, :]
    chs[0:1, :] = first_decay * span[0:1, :]

    half_i = lax.broadcasted_iota(jnp.int32, (RH, EH * CP), 0)
    half_j = lax.broadcasted_iota(jnp.int32, (RH, EH * CP), 1)
    slot_of = half_j & (CP - 1)
    dense = jnp.where(slot_of < CAP, (half_j >> 4) * CAP + slot_of, -1)
    sel = (half_i == dense).astype(BF)

    took(recv1.at[pl.ds(1, SPN - 1)], p1_r)
    for h in range(2):
        got = recv1[pl.ds(h * EH, EH)].reshape(EH * CP, 2 * LANES)
        kept = dot(sel, got, 1, 0).astype(BF)
        inf[0, c, pl.ds(h * RH, RH), :] = kept[:, :LANES]
        cotf[0, c, pl.ds(h * RH, RH), :] = kept[:, LANES:]

    bufs = (inf, cotf)
    DIR = (1, -1)

    def hops(di, piece):
        return H if di == piece else H - 1

    def ring(piece, di, h):
        src = (-DIR[di] * h) % NY
        dst = (-DIR[di] * (h + 1)) % NY
        buf = bufs[piece]
        return remote(
            buf.at[src, c], buf.at[dst, c], y_s.at[di, piece, h], y_r.at[di, piece, h], at_y(DIR[di])
        )

    def across(piece, slot):
        buf = bufs[piece]
        return remote(
            buf.at[slot, c], buf.at[slot, c], d_s.at[piece, slot], d_r.at[piece, slot], partner
        )

    for piece in range(2):
        for di in range(2):
            if hops(di, piece):
                ring(piece, di, 0).start()
        across(piece, 0).start()

    acc[...] = jnp.zeros_like(acc)
    hacc[...] = jnp.zeros_like(hacc)

    def y_at(j):
        return lax.rem(y + j, NY)

    def rows_at(j, wide):
        return pl.ds(pl.multiple_of(y_at(j) * wide, wide), wide)

    def forward_chunk(j):
        across(0, j).wait_recv()
        rows_in = jnp.concatenate([inf[j, 0], inf[j, 1]], axis=1)
        acc[...] += dot(rows_in, wgu[rows_at(j, 256), :], 1, 0)
        across(1, j).wait_recv()
        rows_cot = jnp.concatenate([cotf[j, 0], cotf[j, 1]], axis=1)
        hacc[...] += dot(rows_cot, dw[:, rows_at(j, 256)], 1, 1)

    def at_distance(d):
        return sorted({d % NY, -d % NY})

    for h in range(H):
        for piece in range(2):
            for di in range(2):
                if h < hops(di, piece):
                    ring(piece, di, h).wait_recv()
                    if h + 1 < hops(di, piece):
                        ring(piece, di, h + 1).start()
                    across(piece, (-DIR[di] * (h + 1)) % NY).start()
        for j in at_distance(h):
            forward_chunk(j)
    forward_chunk(H)

    for h in range(2):
        at = pl.ds(h * RH, RH)
        gate_act = acc[at, :LANES]
        up_act = acc[at, LANES:]
        hidden_grad = hacc[at, :]
        squash = jax.nn.sigmoid(gate_act)
        silu_gate = gate_act * squash
        hid[at, :] = (silu_gate * up_act).astype(BF)
        grads[at, :LANES] = (
            hidden_grad * up_act * squash * (1.0 + gate_act * (1.0 - squash))
        ).astype(BF)
        grads[at, LANES:] = (hidden_grad * silu_gate).astype(BF)
    swap = remote(grads, grads_p, g_s, g_r, partner)
    swap.start()

    waited = []

    def term(j):
        own = wgu[pl.ds(pl.multiple_of(y_at(j) * 256 + c * LANES, LANES), LANES), :]
        value = dot(grads[...], own, 1, 1)
        if not waited:
            swap.wait_recv()
            took(wpart, wp_r)
            waited.append(1)
        part[j] = value + dot(grads_p[...], wpart[y_at(j)], 1, 1)

    def weight_grads(j):
        rows_in = jnp.concatenate([inf[j, 0], inf[j, 1]], axis=1)
        ogu[rows_at(j, 256), :] = dot(rows_in, grads[...], 0, 0).astype(BF)
        rows_cot = jnp.concatenate([cotf[j, 0], cotf[j, 1]], axis=1)
        odw[:, rows_at(j, 256)] = dot(hid[...], rows_cot, 0, 0).astype(BF)

    def chain(di, half, k):
        return remote(
            rss.at[di, half, k],
            rsr.at[di, half, k],
            q_s.at[di, half, k],
            q_r.at[di, half, k],
            at_y(DIR[di]),
        )

    ready = set()

    def need(j):
        if j not in ready:
            ready.add(j)
            term(j)

    left = list(range(NY))
    for k in range(H + 1):
        for half, di in ((0, 0), (1, 1), (1, 0), (0, 1)):
            n = hops(di, half)
            if k < n:
                j = (DIR[di] * (n - k)) % NY
                need(j)
                value = part[j, pl.ds(half * RH, RH), :]
                if k:
                    chain(di, half, k - 1).wait_recv()
                    value = value + rsr[di, half, k - 1].astype(F32)
                rss[di, half, k] = value.astype(BF)
                chain(di, half, k).start()
        if k < H:
            for half, di in ((0, 0), (1, 1), (1, 0), (0, 1)):
                n = hops(di, half)
                if k + 1 < n:
                    need((DIR[di] * (n - k - 1)) % NY)
            for j in left[: -(-NY // H)]:
                weight_grads(j)
            left = left[-(-NY // H) :]
    need(0)
    outs = [
        pltpu.make_async_copy(ogu.at[:, pl.ds(0, LANES)], gwg_hbm, o_sem.at[0]),
        pltpu.make_async_copy(ogu.at[:, pl.ds(LANES, LANES)], uwg_hbm, o_sem.at[1]),
        pltpu.make_async_copy(odw, dwg_hbm, o_sem.at[2]),
    ]
    for half in range(2):
        value = part[0, pl.ds(half * RH, RH), :]
        for di in range(2):
            n = hops(di, half)
            if n:
                chain(di, half, n - 1).wait_recv()
                value = value + rsr[di, half, n - 1].astype(F32)
        spread = dot(sel, value.astype(BF), 0, 0).astype(BF)
        send5[pl.ds(half * EH, EH)] = spread.reshape(EH, CP, LANES)
    recv5[0] = send5[0]
    all_sent(lambda k: send5.at[k], lambda k: recv5.at[k], p5_s, p5_r, 1)
    for out in outs:
        out.start()
    took(recv5.at[pl.ds(1, SPN - 1)], p5_r)
    returned = dot(onehot[...], recv5[...].reshape(E * CP, LANES), 1, 0)
    mixf[0, c] = (returned + cot_ref[...].astype(F32)).astype(BF)

    def mix_to(j):
        dst = (-j) % NY
        return remote(mixf.at[0, c], mixf.at[dst, c], m_s.at[dst], m_r.at[dst], at_y(j))

    def mix_across(slot):
        return remote(mixf.at[slot, c], mixf.at[slot, c], md_s.at[slot], md_r.at[slot], partner)

    order = [0]
    for d in range(1, H + 1):
        order += at_distance(d)
    for j in order[:0:-1]:
        mix_to(j).start()
    mix_across(0).start()
    sg[...] = jnp.zeros_like(sg)

    def mixer_chunk(j):
        mix_across(j).wait_recv()
        rows_mix = jnp.concatenate([mixf[j, 0], mixf[j, 1]], axis=1)
        outer = dot(rows_mix, rec[...], 0, 0).astype(BF)
        xsend[j] = outer.reshape(NX, 256 // NX, LANES)
        for dx in range(1, NX):
            to = lax.rem(x + dx, NX)
            remote(
                xsend.at[j, to], xrecv.at[dx, j], x_s, x_r, (z * NX + to, t)
            ).start()
        sg[...] += dot(rows_mix, op[:, rows_at(j, 256)], 1, 1)

    behind = None
    for j in order:
        if j:
            mix_to((-j) % NY).wait_recv()
            mix_across(j).start()
        if behind is not None:
            mixer_chunk(behind)
        behind = j
    mixer_chunk(behind)

    local = sg[...]
    for k in range(n_levels):
        local = local + levels[k] * pltpu.roll(local, TD - (1 << k), 0)
    chs[1:2, :] = first_decay * local[0:1, :]
    all_sent(lambda k: chs, lambda k: chr_.at[k], c_s, c_r, -1)

    took(xrecv.at[pl.ds(1, NX - 1)], x_r)
    mine = None
    for dz in range(NZ):
        to_z = lax.rem(z + dz, NZ)
        j = lax.rem(to_z - y + NY, NY)
        total = xsend[j, x].astype(F32)
        for dx in range(1, NX):
            total = total + xrecv[dx, j].astype(F32)
        if dz == 0:
            mine = total
        else:
            zsend[dz] = total.astype(BF)
            remote(zsend.at[dz], zrecv.at[dz], z_s, z_r, (to_z * NX + x, t)).start()

    took(chr_.at[pl.ds(1, SPN - 1)], c_r)
    entering = jnp.zeros((1, LANES), F32)
    for k in range(SPN - 1, 0, -1):
        entering = jnp.where(s + k < SPN, chr_[k, 1:2, :] + chr_[k, 0:1, :] * entering, entering)
    carried = local + through[...] * entering
    rvg_ref[...] = (carried * coef[0]).astype(BF)
    ipg_ref[...] = (carried * coef[1]).astype(BF)
    rpg_ref[...] = (carried * coef[2]).astype(BF)

    took(zrecv.at[pl.ds(1, NZ - 1)], z_r)
    for dz in range(1, NZ):
        mine = mine + zrecv[dz].astype(F32)
    opg_ref[...] = mine

    took(recv1.at[pl.ds(1, SPN - 1)], p1_s)
    took(wpart, wp_s)
    for piece in range(2):
        for di in range(2):
            for h in range(hops(di, piece)):
                ring(piece, di, h).wait_send()
                chain(di, piece, h).wait_send()
        for j in range(NY):
            across(piece, j).wait_send()
    swap.wait_send()
    took(recv5.at[pl.ds(1, SPN - 1)], p5_s)
    for j in range(1, NY):
        mix_to(j).wait_send()
    for j in range(NY):
        mix_across(j).wait_send()
    took(xrecv.at[pl.ds(1, NX - 1)], x_s)
    took(zrecv.at[pl.ds(1, NZ - 1)], z_s)
    took(chr_.at[pl.ds(1, SPN - 1)], c_s)
    for out in outs:
        out.wait()


def solution(mesh):
    SPN, TPN = mesh.shape["sp"], mesh.shape["tp"]
    NX = 4 if SPN == 32 else 2
    NZ, NY = SPN // NX, TPN // 2

    def per_device(
        ffn_input,
        out_grad,
        routes,
        route_weight,
        gate_w,
        up_w,
        down_w,
        out_proj,
        rec_value,
        rate_pre,
        input_pre,
        prev_state,
        decay_param,
    ):
        TD, top = routes.shape
        E = SPN
        CAP = 5 * top * TD // (4 * E)
        R = E * CAP
        RH = R // 2
        D = gate_w.shape[1]
        H = NY // 2
        CP = SLOT_PAD
        vmem = pl.BlockSpec(memory_space=pltpu.VMEM)
        hbm = pl.BlockSpec(memory_space=pl.ANY)
        dma = pltpu.SemaphoreType.DMA
        levels = TD.bit_length() - 1
        scratch = [
            pltpu.VMEM((D, 256), BF),
            pltpu.VMEM((NY, LANES, 256), BF),
            pltpu.VMEM((LANES, D), BF),
            pltpu.VMEM((LANES, D), BF),
            pltpu.VMEM((TD, E * CP), BF),
            pltpu.VMEM((E, CP, 256), BF),
            pltpu.VMEM((E, CP, 256), BF),
            pltpu.VMEM((NY, 2, R, LANES), BF),
            pltpu.VMEM((NY, 2, R, LANES), BF),
            pltpu.VMEM((R, 256), F32),
            pltpu.VMEM((R, LANES), F32),
            pltpu.VMEM((R, 256), BF),
            pltpu.VMEM((R, 256), BF),
            pltpu.VMEM((R, LANES), BF),
            pltpu.VMEM((NY, R, LANES), F32),
            pltpu.VMEM((2, 2, H, RH, LANES), BF),
            pltpu.VMEM((2, 2, H, RH, LANES), BF),
            pltpu.VMEM((E, CP, LANES), BF),
            pltpu.VMEM((E, CP, LANES), BF),
            pltpu.VMEM((NY, 2, TD, LANES), BF),
            pltpu.VMEM((TD, LANES), F32),
            pltpu.VMEM((levels, TD, LANES), F32),
            pltpu.VMEM((TD, LANES), F32),
            pltpu.VMEM((3, TD, LANES), F32),
            pltpu.VMEM((TD, LANES), BF),
            pltpu.VMEM((NY, NX, 256 // NX, LANES), BF),
            pltpu.VMEM((NX, NY, 256 // NX, LANES), BF),
            pltpu.VMEM((NZ, 256 // NX, LANES), BF),
            pltpu.VMEM((NZ, 256 // NX, LANES), BF),
            pltpu.VMEM((2, LANES), F32),
            pltpu.VMEM((SPN, 2, LANES), F32),
            pltpu.VMEM((D, 256), BF),
            pltpu.VMEM((LANES, D), BF),
            dma((4,)),
            dma((3,)),
            dma,
            dma,
            dma,
            dma,
            dma((2, 2, H)),
            dma((2, 2, H)),
            dma((2, NY)),
            dma((2, NY)),
            dma,
            dma,
            dma((2, 2, H)),
            dma((2, 2, H)),
            dma,
            dma,
            dma((NY,)),
            dma((NY,)),
            dma((NY,)),
            dma((NY,)),
            dma,
            dma,
            dma,
            dma,
            dma,
            dma,
        ]
        shape = jax.ShapeDtypeStruct
        outs = pl.pallas_call(
            functools.partial(step_kernel, (SPN, NX, NY, E, CAP, TD, R)),
            out_shape=(
                shape((D, LANES), BF),
                shape((D, LANES), BF),
                shape((LANES, D), BF),
                shape((256 // NX, LANES), F32),
                shape((TD, LANES), BF),
                shape((TD, LANES), BF),
                shape((TD, LANES), BF),
            ),
            in_specs=[vmem] * 4 + [hbm] * 4 + [vmem] * 5,
            out_specs=[hbm] * 3 + [vmem] * 4,
            scratch_shapes=scratch,
            compiler_params=pltpu.CompilerParams(collective_id=0, has_side_effects=True),
        )(
            ffn_input,
            out_grad,
            routes,
            route_weight,
            gate_w[0],
            up_w[0],
            down_w[0],
            out_proj,
            rec_value,
            rate_pre,
            input_pre,
            prev_state,
            decay_param.reshape(1, -1),
        )
        return (outs[0][None], outs[1][None], outs[2][None], *outs[3:])

    tokens = P("sp", "tp")
    placed = (
        tokens,
        tokens,
        P("sp", None),
        P("sp", None),
        P("sp", None, "tp"),
        P("sp", None, "tp"),
        P("sp", "tp", None),
        P("tp", None),
        tokens,
        tokens,
        tokens,
        tokens,
        P("tp"),
    )
    return jax.shard_map(
        per_device,
        mesh=mesh,
        in_specs=placed,
        out_specs=(
            P("sp", None, "tp"),
            P("sp", None, "tp"),
            P("sp", "tp", None),
            tokens,
            tokens,
            tokens,
            tokens,
        ),
        check_vma=False,
    )
```

```python
import contextlib
import functools

import jax
import jax.numpy as jnp
from jax import lax
from jax.experimental import pallas as pl
from jax.experimental.pallas import tpu as pltpu
from jax.sharding import PartitionSpec as P


MESH = pl.DeviceIdType.MESH
F32 = jnp.float32
BF = jnp.bfloat16
decay_scale = 8.0
SCOPES = False
SLOT_PAD = 16
LANES = 128


def dot(a, b, ca, cb):
    return lax.dot_general(a, b, (((ca,), (cb,)), ((), ())), preferred_element_type=F32)


PHASE = contextlib.ExitStack()


def mark(name):
    if SCOPES:
        PHASE.close()
        if name:
            PHASE.enter_context(jax.named_scope(name))


def expm1_neg(v):
    near = jnp.ones_like(v)
    for n in range(9, 1, -1):
        near = 1.0 + v * near * (1.0 / n)
    return jnp.where(v > -0.5, v * near, jnp.exp(v) - 1.0)


def step_kernel(
    dims,
    x_hbm,
    cot_hbm,
    rt_hbm,
    rw_hbm,
    gw_hbm,
    uw_hbm,
    dw_hbm,
    op_hbm,
    rv_hbm,
    rp_hbm,
    ip_hbm,
    ps_hbm,
    dp_hbm,
    gwg_ref,
    uwg_ref,
    dwg_ref,
    opg_ref,
    rvg_ref,
    rpg_ref,
    ipg_ref,
    x_ref,
    cot_ref,
    rt_ref,
    rw_ref,
    rv_ref,
    rp_ref,
    ip_ref,
    ps_ref,
    dp_ref,
    wgu,
    wpart,
    dw,
    op,
    onehot,
    send1,
    recv1,
    inf,
    cotf,
    acc,
    hacc,
    grads,
    grads_p,
    hid,
    part,
    rss,
    rsr,
    send5,
    recv5,
    mixf,
    sg,
    levels,
    through,
    coef,
    rec,
    xsend,
    xrecv,
    zsum,
    zsend,
    zrecv,
    chs,
    chr_,
    w_sem,
    wp_s,
    wp_r,
    p1_s,
    p1_r,
    y_s,
    y_r,
    d_s,
    d_r,
    g_s,
    g_r,
    q_s,
    q_r,
    p5_s,
    p5_r,
    m_s,
    m_r,
    md_s,
    md_r,
    x_s,
    x_r,
    z_s,
    z_r,
    c_s,
    c_r,
):
    SPN, NX, NY, E, CAP, TD, R = dims
    NZ = SPN // NX
    RH = R // 2
    EH = E // 2
    CP = SLOT_PAD
    H = NY // 2
    s = lax.axis_index("sp")
    t = lax.axis_index("tp")
    y = t // 2
    c = t % 2
    z = s // NX
    x = s % NX

    def remote(src, dst, ss, rs, dev):
        return pltpu.make_async_remote_copy(
            src_ref=src, dst_ref=dst, send_sem=ss, recv_sem=rs, device_id=dev, device_id_type=MESH
        )

    def at_y(j):
        return (s, lax.rem(y + j + NY, NY) * 2 + c)

    partner = (s, y * 2 + 1 - c)

    def at_sp(j):
        return (lax.rem(s + j + SPN, SPN), t)

    def took(ref, sem):
        pltpu.make_async_copy(ref, ref, sem).wait()

    mark("start")
    loads = [
        pltpu.make_async_copy(src, dst, w_sem.at[n])
        for n, (src, dst) in enumerate(
            (
                (rt_hbm, rt_ref),
                (rw_hbm, rw_ref),
                (x_hbm, x_ref),
                (cot_hbm, cot_ref),
                (gw_hbm, wgu.at[:, pl.ds(0, LANES)]),
                (uw_hbm, wgu.at[:, pl.ds(LANES, LANES)]),
                (rv_hbm, rv_ref),
                (rp_hbm, rp_ref),
                (ip_hbm, ip_ref),
                (ps_hbm, ps_ref),
                (dp_hbm, dp_ref),
                (dw_hbm, dw),
                (op_hbm, op),
            )
        )
    ]
    for load in loads:
        load.start()

    barrier = pltpu.get_barrier_semaphore()

    def greet(k, carry):
        pl.semaphore_signal(barrier, inc=1, device_id=at_sp(k), device_id_type=MESH)
        return carry

    lax.fori_loop(1, SPN, greet, 0)
    for j in range(1, NY):
        pl.semaphore_signal(barrier, inc=1, device_id=at_y(j), device_id_type=MESH)
    pl.semaphore_signal(barrier, inc=1, device_id=partner, device_id_type=MESH)
    for load in loads[:4]:
        load.wait()

    mark("route")
    rows = lax.broadcasted_iota(jnp.int32, (TD, TD), 0)
    cols = lax.broadcasted_iota(jnp.int32, (TD, TD), 1)
    earlier = (rows < cols).astype(BF)
    ids = lax.broadcasted_iota(jnp.int32, (E, TD), 0)
    r0, r1 = rt_ref[0:1, :], rt_ref[1:2, :]
    marks0 = (ids == r0).astype(F32)
    marks1 = (ids == r1).astype(F32)
    before = dot((marks0 + marks1).astype(BF), earlier, 1, 0)
    slots = lax.broadcasted_iota(jnp.int32, (E * CP, TD), 0)

    def picks(r, marks):
        rank = jnp.sum(before * marks, axis=0, keepdims=True).astype(jnp.int32)
        back_x = x - lax.rem(r, NX)
        back_x = jnp.where(back_x < 0, back_x + NX, back_x)
        back_z = z - lax.div(r, NX)
        back_z = jnp.where(back_z < 0, back_z + NZ, back_z)
        turn = jnp.where(back_z <= NZ // 2, jnp.maximum(2 * back_z - 1, 0), 2 * (NZ - back_z))
        away = turn * NX + back_x
        return (slots == away * CP + rank).astype(F32)

    pick0 = picks(r0, marks0)
    pick1 = picks(r1, marks1)
    both = (pick0 + pick1).astype(BF)
    onehot[...] = both
    weight = jnp.sum(pick0 * rw_ref[0:1, :] + pick1 * rw_ref[1:2, :], axis=1, keepdims=True)
    row_in = dot(both, x_ref[...], 1, 0).astype(BF)
    row_cot = (weight * dot(both, cot_ref[...], 1, 0)).astype(BF)
    send1[:, :, 0:LANES] = row_in.reshape(E, CP, LANES)
    send1[:, :, LANES:] = row_cot.reshape(E, CP, LANES)
    recv1[0] = send1[0]

    mark("barrier")
    pl.semaphore_wait(barrier, SPN - 1 + NY - 1 + 1)

    def all_sent(src_of, dst_of, ss, rs, sign):
        def go(k):
            remote(src_of(k), dst_of(k), ss, rs, at_sp(sign * k)).start()

        def pair(k, carry):
            go(k)
            go(SPN - k)
            return carry

        lax.fori_loop(1, SPN // 2, pair, 0)
        go(SPN // 2)

    mark("p1send")
    def offsets(half):
        turns = range(NZ // 2) if half == 0 else range(NZ // 2, NZ)
        if NZ == 1:
            turns = ()
        for turn in reversed(turns):
            kz = (turn + 1) // 2 if turn % 2 or turn == 0 else NZ - turn // 2
            for kx in sorted(range(NX), key=lambda k: -min(k, NX - k)):
                if turn or kx:
                    yield turn * NX + kx, kz, kx

    def exchange(send, recv, ss, rs, half, sign):
        for at, kz, kx in offsets(half):
            to = lax.rem(z + sign * kz + NZ, NZ) * NX + lax.rem(x + sign * kx + NX, NX)
            remote(send.at[at], recv.at[at], ss, rs.at[half], (to, t)).start()

    def exchanged(recv, rs, half):
        first = 1 if half == 0 else EH
        if EH * (half + 1) > first:
            took(recv.at[pl.ds(first, EH * (half + 1) - first)], rs.at[half])

    for half in range(2):
        exchange(send1, recv1, p1_s, p1_r, half, -1)

    loads[4].wait()
    loads[5].wait()
    for j in range(NY):
        remote(
            wgu.at[pl.ds(pl.multiple_of(j * 256 + (1 - c) * LANES, LANES), LANES), :],
            wpart.at[j],
            wp_s,
            wp_r,
            partner,
        ).start()
    for load in loads[6:]:
        load.wait()

    mark("coef")
    decay_speed = jnp.log1p(jnp.exp(-dp_ref[...]))
    rate = jax.nn.sigmoid(rp_ref[...].astype(F32))
    inlet = jax.nn.sigmoid(ip_ref[...].astype(F32))
    signal = rv_ref[...].astype(F32)
    prev = ps_ref[...].astype(F32)
    log_decay = -decay_scale * rate * decay_speed
    decay = jnp.exp(log_decay)
    scale_in = jnp.sqrt(-expm1_neg(2.0 * log_decay))
    rec[...] = (decay * prev + scale_in * inlet * signal).astype(BF)
    gain = scale_in * inlet
    coef[0] = gain
    coef[1] = gain * signal * (1.0 - inlet)
    slope = decay * prev - inlet * signal * decay * decay / scale_in
    coef[2] = slope * (-decay_scale * decay_speed) * rate * (1.0 - rate)
    tok = lax.broadcasted_iota(jnp.int32, (TD, LANES), 0)
    span = jnp.where(tok < TD - 1, pltpu.roll(decay, TD - 1, 0), 1.0)
    n_levels = TD.bit_length() - 1
    for k in range(n_levels):
        inside = tok < TD - (1 << k)
        levels[k] = jnp.where(inside, span, 0.0)
        span = span * jnp.where(inside, pltpu.roll(span, TD - (1 << k), 0), 1.0)
    through[...] = span
    first_decay = decay[0:1, :]
    chs[0:1, :] = first_decay * span[0:1, :]

    half_i = lax.broadcasted_iota(jnp.int32, (RH, EH * CP), 0)
    half_j = lax.broadcasted_iota(jnp.int32, (RH, EH * CP), 1)
    slot_of = half_j & (CP - 1)
    dense = jnp.where(slot_of < CAP, (half_j >> 4) * CAP + slot_of, -1)
    sel = (half_i == dense).astype(BF)

    bufs = (inf, cotf)
    DIR = (1, -1)

    def hops(di, kind):
        return H if di == kind else H - 1

    def half_of(half):
        return pl.ds(half * RH, RH)

    def ring(half, kind, di, h):
        src = (-DIR[di] * h) % NY
        dst = (-DIR[di] * (h + 1)) % NY
        piece = half * 2 + kind
        return remote(
            bufs[kind].at[src, c, half_of(half), :],
            bufs[kind].at[dst, c, half_of(half), :],
            y_s.at[di, piece, h],
            y_r.at[di, piece, h],
            at_y(DIR[di]),
        )

    def across(half, kind, slot):
        ref = bufs[kind].at[slot, c, half_of(half), :]
        piece = half * 2 + kind
        return remote(ref, ref, d_s.at[piece, slot], d_r.at[piece, slot], partner)

    def y_at(j):
        return lax.rem(y + j, NY)

    def rows_at(j, wide):
        return pl.ds(pl.multiple_of(y_at(j) * wide, wide), wide)

    def at_distance(d):
        return sorted({d % NY, -d % NY})

    def begin(half):
        exchanged(recv1, p1_r, half)
        got = recv1[pl.ds(half * EH, EH)].reshape(EH * CP, 2 * LANES)
        kept = dot(sel, got, 1, 0).astype(BF)
        inf[0, c, half_of(half), :] = kept[:, :LANES]
        cotf[0, c, half_of(half), :] = kept[:, LANES:]
        for kind in range(2):
            for di in range(2):
                if hops(di, kind):
                    ring(half, kind, di, 0).start()
            across(half, kind, 0).start()

    def arrive(half, h):
        for kind in range(2):
            for di in range(2):
                if h <= hops(di, kind):
                    ring(half, kind, di, h - 1).wait_recv()
                    if h < hops(di, kind):
                        ring(half, kind, di, h).start()
                    across(half, kind, (-DIR[di] * h) % NY).start()

    def consume(half, d):
        for j in at_distance(d):
            at = half_of(half)
            across(half, 0, j).wait_recv()
            rows_in = jnp.concatenate([inf[j, 0, at, :], inf[j, 1, at, :]], axis=1)
            value = dot(rows_in, wgu[rows_at(j, 256), :], 1, 0)
            across(half, 1, j).wait_recv()
            rows_cot = jnp.concatenate([cotf[j, 0, at, :], cotf[j, 1, at, :]], axis=1)
            value_h = dot(rows_cot, dw[:, rows_at(j, 256)], 1, 1)
            if d:
                acc[at, :] += value
                hacc[at, :] += value_h
            else:
                acc[at, :] = value
                hacc[at, :] = value_h

    def swap(half):
        at = half_of(half)
        return remote(grads.at[at, :], grads_p.at[at, :], g_s.at[half], g_r.at[half], partner)

    def activate(half):
        at = half_of(half)
        gate_act = acc[at, :LANES]
        up_act = acc[at, LANES:]
        hidden_grad = hacc[at, :]
        squash = jax.nn.sigmoid(gate_act)
        silu_gate = gate_act * squash
        grads[at, :LANES] = (
            hidden_grad * up_act * squash * (1.0 + gate_act * (1.0 - squash))
        ).astype(BF)
        grads[at, LANES:] = (hidden_grad * silu_gate).astype(BF)
        swap(half).start()
        hid[at, :] = (silu_gate * up_act).astype(BF)

    ready = set()

    def need(half, j):
        if (half, j) in ready:
            return
        at = half_of(half)
        own = wgu[pl.ds(pl.multiple_of(y_at(j) * 256 + c * LANES, LANES), LANES), :]
        value = dot(grads[at, :], own, 1, 1)
        if not ready:
            took(wpart, wp_r)
        if not any(done == half for done, _ in ready):
            swap(half).wait_recv()
        ready.add((half, j))
        part[j, at, :] = value + dot(grads_p[at, :], wpart[y_at(j)], 1, 1)

    def chain(di, half, k):
        return remote(
            rss.at[di, half, k],
            rsr.at[di, half, k],
            q_s.at[di, half, k],
            q_r.at[di, half, k],
            at_y(DIR[di]),
        )

    def target(di, half, k):
        return (DIR[di] * (hops(di, half) - k)) % NY

    def pass_on(half, k):
        for di in (half, 1 - half):
            if k < hops(di, half):
                j = target(di, half, k)
                need(half, j)
                value = part[j, half_of(half), :]
                if k:
                    chain(di, half, k - 1).wait_recv()
                    value = value + rsr[di, half, k - 1].astype(F32)
                rss[di, half, k] = value.astype(BF)
                chain(di, half, k).start()

    def ahead(half, k):
        for di in (half, 1 - half):
            if k <= hops(di, half):
                need(half, target(di, half, k))

    def finish(half):
        need(half, 0)
        value = part[0, half_of(half), :]
        for di in (1 - half, half):
            n = hops(di, half)
            if n:
                chain(di, half, n - 1).wait_recv()
                value = value + rsr[di, half, n - 1].astype(F32)
        spread = dot(sel, value.astype(BF), 0, 0).astype(BF)
        send5[pl.ds(half * EH, EH)] = spread.reshape(EH, CP, LANES)
        if half == 0:
            recv5[0] = send5[0]
        exchange(send5, recv5, p5_s, p5_r, half, 1)

    def weight_grads(j):
        rows_in = jnp.concatenate([inf[j, 0], inf[j, 1]], axis=1)
        both = dot(rows_in, grads[...], 0, 0).astype(BF)
        gwg_ref[rows_at(j, 256), :] = both[:, :LANES]
        uwg_ref[rows_at(j, 256), :] = both[:, LANES:]
        rows_cot = jnp.concatenate([cotf[j, 0], cotf[j, 1]], axis=1)
        dwg_ref[:, rows_at(j, 256)] = dot(hid[...], rows_cot, 0, 0).astype(BF)

    mark("p1wait")
    begin(0)
    mark("p2")
    for i in range(1, H + 1):
        arrive(0, i)
        if i == 1:
            mark("p1waitB")
            begin(1)
            mark("p2B")
        else:
            arrive(1, i - 1)
        consume(0, i - 1)
        if i == H:
            consume(0, H)
            activate(0)
        if i >= 2:
            consume(1, i - 2)
    mark("p2last")
    arrive(1, H)
    consume(1, H - 1)
    mark("p4")
    pass_on(0, 0)
    consume(1, H)
    activate(1)
    ahead(0, 1)
    todo = list(range(NY))
    per = -(-NY // H)
    for k in range(H):
        if k + 1 < H:
            pass_on(0, k + 1)
        else:
            mark("finA")
            finish(0)
            mark("p4B")
        pass_on(1, k)
        if k + 2 <= H:
            ahead(0, k + 2)
        ahead(1, k + 1)
        for j in todo[:per]:
            weight_grads(j)
        todo = todo[per:]
    mark("finB")
    finish(1)
    mark("p5")
    for half in range(2):
        exchanged(recv5, p5_r, half)
    returned = dot(onehot[...], recv5[...].reshape(E * CP, LANES), 0, 0)
    mixf[0, c] = (returned + cot_ref[...].astype(F32)).astype(BF)

    mark("p6")
    TH = TD // 2
    staged = H == 4

    def mix_copy(src, dst, to, tokens):
        first, count = tokens
        at = pl.ds(first, count)
        n = dst * 2 + (first > 0)
        return remote(
            mixf.at[src % NY, c, at, :], mixf.at[dst % NY, c, at, :], m_s.at[n], m_r.at[n], at_y(to)
        )

    def mix_across(slot):
        ref = mixf.at[slot, c]
        return remote(ref, ref, md_s.at[slot], md_r.at[slot], partner)

    whole = (0, TD)
    if staged:
        direct = [2, NY - 2, 1, NY - 1]
    else:
        direct = [j for d in range(H, 0, -1) for j in at_distance(d)]
    mix_sends = []
    mix_recv = {}

    def mix_send(src, dst, to, tokens):
        copy = mix_copy(src, dst, to, tokens)
        mix_sends.append(copy)
        mix_recv.setdefault(dst, []).append(copy)
        return copy

    for j in direct:
        mix_send(0, -j % NY, j, whole).start()
    mix_across(0).start()
    passing = {}
    if staged:
        passing[NY - 2] = [
            mix_send(NY - 2, NY - 4, 2, (0, TH)),
            mix_send(NY - 2, NY - 3, 1, whole),
        ]
        passing[2] = [mix_send(2, 4, -2, (TH, TH)), mix_send(2, 3, -1, whole)]

    def mixer_chunk(j):
        if j:
            mix_across(j).wait_recv()
        else:
            mix_across(0).wait_recv()
        rows_mix = jnp.concatenate([mixf[j, 0], mixf[j, 1]], axis=1)
        outer = dot(rows_mix, rec[...], 0, 0).astype(BF)
        xsend[j] = outer.reshape(NX, 256 // NX, LANES)
        for dx in range(1, NX):
            to = lax.rem(x + dx, NX)
            remote(
                xsend.at[j, to], xrecv.at[j, dx], x_s, x_r.at[j], (z * NX + to, t)
            ).start()
        value = dot(rows_mix, op[:, rows_at(j, 256)], 1, 1)
        if j:
            sg[...] += value
        else:
            sg[...] = value

    def down_z(j):
        if NX > 1:
            took(xrecv.at[j, pl.ds(1, NX - 1)], x_r.at[j])
        total = xsend[j, x].astype(F32)
        for dx in range(1, NX):
            total = total + xrecv[j, dx].astype(F32)
        zsum[j] = total
        zsend[j] = total.astype(BF)
        to_z = y_at(j)
        dz = lax.rem(to_z - z + NZ, NZ)

        @pl.when(dz != 0)
        def _():
            remote(zsend.at[j], zrecv.at[dz], z_s, z_r, (to_z * NX + x, t)).start()

    order = [0]
    for d in range(1, H + 1):
        order += at_distance(d)
    if staged:
        waits = [2, NY - 2, 1, NY - 1, 3, NY - 3, 4]
    else:
        waits = order[1:]
    done = [0]
    for j in waits:
        for copy in mix_recv[j]:
            copy.wait_recv()
        for copy in passing.get(j, ()):
            copy.start()
        mix_across(j).start()
        mixer_chunk(done[-1])
        done.append(j)
    mixer_chunk(done[-1])

    mark("scan")
    local = sg[...]
    for k in range(n_levels):
        local = local + levels[k] * pltpu.roll(local, TD - (1 << k), 0)
    chs[1:2, :] = first_decay * local[0:1, :]
    all_sent(lambda k: chs, lambda k: chr_.at[k], c_s, c_r, -1)

    mark("xwait")
    for j in done:
        down_z(j)
    mine = zsum[lax.rem(z - y + NZ, NZ)]

    mark("cwait")
    took(chr_.at[pl.ds(1, SPN - 1)], c_r)
    entering = jnp.zeros((1, LANES), F32)
    for k in range(SPN - 1, 0, -1):
        entering = jnp.where(s + k < SPN, chr_[k, 1:2, :] + chr_[k, 0:1, :] * entering, entering)
    carried = local + through[...] * entering
    rvg_ref[...] = (carried * coef[0]).astype(BF)
    ipg_ref[...] = (carried * coef[1]).astype(BF)
    rpg_ref[...] = (carried * coef[2]).astype(BF)

    mark("zwait")
    took(zrecv.at[pl.ds(1, NZ - 1)], z_r)
    for dz in range(1, NZ):
        mine = mine + zrecv[dz].astype(F32)
    opg_ref[...] = mine

    mark("drain")
    took(recv1.at[pl.ds(1, SPN - 1)], p1_s)
    took(wpart, wp_s)
    for half in range(2):
        for di in range(2):
            for kind in range(2):
                for h in range(hops(di, kind)):
                    ring(half, kind, di, h).wait_send()
            for k in range(hops(di, half)):
                chain(di, half, k).wait_send()
        for kind in range(2):
            for j in range(NY):
                across(half, kind, j).wait_send()
        swap(half).wait_send()
    took(recv5.at[pl.ds(1, SPN - 1)], p5_s)
    for copy in mix_sends:
        copy.wait_send()
    for j in range(NY):
        mix_across(j).wait_send()
    if NX > 1:
        took(xrecv.at[:, pl.ds(1, NX - 1)], x_s)
    took(zrecv.at[pl.ds(1, NZ - 1)], z_s)
    took(chr_.at[pl.ds(1, SPN - 1)], c_s)
    mark(None)


def tail_kernel(*refs):
    copies = [
        pltpu.make_async_copy(refs[n], refs[7 + n], refs[14].at[n]) for n in range(7)
    ]
    for copy in copies:
        copy.start()
    for copy in copies:
        copy.wait()


def solution(mesh):
    SPN, TPN = mesh.shape["sp"], mesh.shape["tp"]
    NX = {32: 4, 8: 2, 4: 2}[SPN]
    NZ, NY = SPN // NX, TPN // 2

    def per_device(
        ffn_input,
        out_grad,
        routes,
        route_weight,
        gate_w,
        up_w,
        down_w,
        out_proj,
        rec_value,
        rate_pre,
        input_pre,
        prev_state,
        decay_param,
    ):
        TD, top = routes.shape
        E = SPN
        CAP = 5 * top * TD // (4 * E)
        R = E * CAP
        RH = R // 2
        D = gate_w.shape[1]
        H = NY // 2
        CP = SLOT_PAD
        vmem = pl.BlockSpec(memory_space=pltpu.VMEM)
        hbm = pl.BlockSpec(memory_space=pltpu.HBM)
        anywhere = pl.BlockSpec(memory_space=pl.ANY)
        dma = pltpu.SemaphoreType.DMA
        levels = TD.bit_length() - 1
        tile = pltpu.VMEM((TD, LANES), BF)
        scratch = [
            tile,
            tile,
            pltpu.VMEM((top, TD), jnp.int32),
            pltpu.VMEM((top, TD), F32),
            tile,
            tile,
            tile,
            tile,
            pltpu.VMEM((1, LANES), F32),
            pltpu.VMEM((D, 256), BF),
            pltpu.VMEM((NY, LANES, 256), BF),
            pltpu.VMEM((LANES, D), BF),
            pltpu.VMEM((LANES, D), BF),
            pltpu.VMEM((E * CP, TD), BF),
            pltpu.VMEM((E, CP, 256), BF),
            pltpu.VMEM((E, CP, 256), BF),
            pltpu.VMEM((NY, 2, R, LANES), BF),
            pltpu.VMEM((NY, 2, R, LANES), BF),
            pltpu.VMEM((R, 256), F32),
            pltpu.VMEM((R, LANES), F32),
            pltpu.VMEM((R, 256), BF),
            pltpu.VMEM((R, 256), BF),
            pltpu.VMEM((R, LANES), BF),
            pltpu.VMEM((NY, R, LANES), F32),
            pltpu.VMEM((2, 2, H, RH, LANES), BF),
            pltpu.VMEM((2, 2, H, RH, LANES), BF),
            pltpu.VMEM((E, CP, LANES), BF),
            pltpu.VMEM((E, CP, LANES), BF),
            pltpu.VMEM((NY, 2, TD, LANES), BF),
            pltpu.VMEM((TD, LANES), F32),
            pltpu.VMEM((levels, TD, LANES), F32),
            pltpu.VMEM((TD, LANES), F32),
            pltpu.VMEM((3, TD, LANES), F32),
            pltpu.VMEM((TD, LANES), BF),
            pltpu.VMEM((NY, NX, 256 // NX, LANES), BF),
            pltpu.VMEM((NY, NX, 256 // NX, LANES), BF),
            pltpu.VMEM((NZ, 256 // NX, LANES), F32),
            pltpu.VMEM((NZ, 256 // NX, LANES), BF),
            pltpu.VMEM((NZ, 256 // NX, LANES), BF),
            pltpu.VMEM((2, LANES), F32),
            pltpu.VMEM((SPN, 2, LANES), F32),
            dma((13,)),
            dma,
            dma,
            dma,
            dma((2,)),
            dma((2, 4, H)),
            dma((2, 4, H)),
            dma((4, NY)),
            dma((4, NY)),
            dma((2,)),
            dma((2,)),
            dma((2, 2, H)),
            dma((2, 2, H)),
            dma,
            dma((2,)),
            dma((2 * NY,)),
            dma((2 * NY,)),
            dma((NY,)),
            dma((NY,)),
            dma,
            dma((NY,)),
            dma,
            dma,
            dma,
            dma,
        ]
        shape = jax.ShapeDtypeStruct
        outs = pl.pallas_call(
            functools.partial(step_kernel, (SPN, NX, NY, E, CAP, TD, R)),
            out_shape=(
                shape((D, LANES), BF),
                shape((D, LANES), BF),
                shape((LANES, D), BF),
                shape((256 // NX, LANES), F32),
                shape((TD, LANES), BF),
                shape((TD, LANES), BF),
                shape((TD, LANES), BF),
            ),
            in_specs=[hbm] * 13,
            out_specs=[vmem] * 7,
            scratch_shapes=scratch,
            compiler_params=pltpu.CompilerParams(
                collective_id=0, has_side_effects=True, vmem_limit_bytes=24 * 1024 * 1024
            ),
        )(*[pltpu.with_memory_space_constraint(v, pltpu.HBM) for v in (
            ffn_input,
            out_grad,
            routes.T,
            route_weight.T,
            gate_w[0],
            up_w[0],
            down_w[0],
            out_proj,
            rec_value,
            rate_pre,
            input_pre,
            prev_state,
            decay_param.reshape(1, -1),
        )])
        outs = pl.pallas_call(
            tail_kernel,
            out_shape=tuple(shape(o.shape, o.dtype) for o in outs),
            in_specs=[anywhere] * 7,
            out_specs=[hbm] * 7,
            scratch_shapes=[dma((7,))],
            compiler_params=pltpu.CompilerParams(vmem_limit_bytes=1024 * 1024),
        )(*outs)
        return (outs[0][None], outs[1][None], outs[2][None], *outs[3:])

    tokens = P("sp", "tp")
    placed = (
        tokens,
        tokens,
        P("sp", None),
        P("sp", None),
        P("sp", None, "tp"),
        P("sp", None, "tp"),
        P("sp", "tp", None),
        P("tp", None),
        tokens,
        tokens,
        tokens,
        tokens,
        P("tp"),
    )
    return jax.shard_map(
        per_device,
        mesh=mesh,
        in_specs=placed,
        out_specs=(
            P("sp", None, "tp"),
            P("sp", None, "tp"),
            P("sp", "tp", None),
            tokens,
            tokens,
            tokens,
            tokens,
        ),
        check_vma=False,
    )
```
